512 devices in a mesh: sp: 32 (over z, core), tp: 16 (over y, x).
Axes of the slice: x: 4, y: 4, z: 16, core: 2. Of those that a mesh axis runs over, the one named last changes fastest.
Arguments:
- residual_in: bfloat16 [4096, 2048], P('sp', 'tp'), may hold values from -6 to 6
- query_wide: bfloat16 [4096, 2048], P('sp', 'tp'), may hold values from -6 to 6
- narrow_head_query: bfloat16 [4096, 1024], P('sp', 'tp'), may hold values from -6 to 6
- forget_wide: bfloat16 [4096, 2048], P('sp', 'tp'), may hold values from -6 to 6
- forget_narrow: bfloat16 [4096, 1024], P('sp', 'tp'), may hold values from -6 to 6
- room_wide: float32 [2048], P('tp'), as said below
- room_narrow: float32 [1024], P('tp'), as said below
- values: bfloat16 [4096, 2048], P('sp', 'tp'), may hold values from -6 to 6
- out_gate: bfloat16 [4096, 2048], P('sp', 'tp'), may hold values from -6 to 6
- head_gain: float32 [2048], P('tp'), may hold values from 0.1 to 1.9
- w_out: bfloat16 [2048, 2048], P(None, 'tp'), may hold values from -0.125 to 0.125
- norm_gain: float32 [2048], P('tp'), may hold values from 0.1 to 1.9
- route_ids: int32 [4096, 2], P('sp'), may hold values from 0 to 31, all different within a row; in each aligned block of 128 rows (0 to 127, 128 to 255, ...) at most 10 rows name the same one
- route_weight: float32 [4096, 2], P('sp'), may hold values from 0.25 to 1
- w_gate: bfloat16 [32, 2048, 4096], P('sp', None, 'tp'), may hold values from -0.125 to 0.125
- w_up: bfloat16 [32, 2048, 4096], P('sp', None, 'tp'), may hold values from -0.125 to 0.125
- w_down: bfloat16 [32, 4096, 2048], P('sp', 'tp'), may hold values from -0.09375 to 0.09375
Outputs:
- layer_out: bfloat16 [4096, 2048], P('sp', 'tp')
The draws below stay inside these ranges and needn't reach their ends.
Inputs may be any that keep to these rules, and one draw needn't show every extreme that they name: `room_wide`: every value is positive and below 0.125. `room_narrow`: every value is positive and below 0.125. `route_ids`: each token names 2 different experts; among the 128 tokens of one index of sp no expert is named more than 10 times, and on some indices one is named exactly 10 times.
All inputs are finite; a program needn't handle non-finite values.
Results may differ from the reference program's by a relative error of at most 0.012.
Values may be sent and summed in bfloat16 or wider, within the bound.
A program may use at most 64 MiB of HBM per device.

```python
import math
import jax
import jax.numpy as jnp
import numpy as np
from jax import lax

D = 2048
PAIRS = 16
DKW = 128
DKN = 64
DV = 64
VAL = 2048
FF = 4096
TOPK = 2
BLOCK = 64
TOK_DEV = 128
TOKENS = 4096
EXPERTS = 32
CAP = 10
N_SP = 32


def slow_heads(room_key):
    pick_key = jax.random.split(room_key, 3)[0]
    slow_share = 0.5
    return jax.random.bernoulli(pick_key, slow_share, (PAIRS, 1))


def forget_draw(key, room_key, key_dim):
    columns = PAIRS * key_dim
    noise_key, device_key, block_key, sign_key = jax.random.split(key, 4)
    noise_term = jnp.clip(jax.random.normal(noise_key, (TOKENS, columns), jnp.float32), -3.0, 3.0)
    span_count = TOKENS // TOK_DEV
    block_count = TOKENS // BLOCK
    per_device = jax.random.uniform(device_key, (span_count, 1, columns), jnp.float32, -3.0, 3.0)
    per_block = jax.random.uniform(block_key, (block_count, 1, columns), jnp.float32, -1.0, 1.0)
    offset_sum = jnp.broadcast_to(per_device, (span_count, TOK_DEV, columns)).reshape(TOKENS, columns)
    offset_sum = offset_sum + jnp.broadcast_to(per_block, (block_count, BLOCK, columns)).reshape(TOKENS, columns)
    slow_head = slow_heads(room_key)
    head_sign = jnp.where(jax.random.bernoulli(sign_key, 0.5, (PAIRS, 1)), 3.0, -3.0)
    head_shift = jnp.broadcast_to(jnp.where(slow_head, head_sign, 0.0), (PAIRS, key_dim)).reshape(1, columns)
    return jnp.clip(noise_term + offset_sum + head_shift, -6.0, 6.0).astype(jnp.bfloat16)


def room_draw(key, key_dim):
    pick_key, slow_key, fast_key = jax.random.split(key, 3)
    slow_head = slow_heads(key)
    slow_rate = jnp.exp(jax.random.uniform(slow_key, (PAIRS, key_dim), jnp.float32, math.log(0.5), math.log(2.0))) / TOKENS
    fast_rate = jnp.exp(jax.random.uniform(fast_key, (PAIRS, key_dim), jnp.float32, math.log(0.04), math.log(0.12)))
    return jnp.where(slow_head, slow_rate, fast_rate).reshape(PAIRS * key_dim).astype(jnp.float32)


def draw_forget_wide(key, part):
    return forget_draw(jax.random.fold_in(key, 11), jax.random.fold_in(key, 21), DKW)


def draw_forget_narrow(key, part):
    return forget_draw(jax.random.fold_in(key, 12), jax.random.fold_in(key, 22), DKN)


def draw_room_wide(key, part):
    return room_draw(jax.random.fold_in(key, 21), DKW)


def draw_room_narrow(key, part):
    return room_draw(jax.random.fold_in(key, 22), DKN)


def levels(stream_key, dims, cuts, least, high):
    level, own = 1.0, jax.random.fold_in(stream_key, 6)
    for dim, parts in cuts:
        heights = jnp.exp(jax.random.uniform(jax.random.fold_in(own, dim), (parts,), jnp.float32, least / len(cuts), high / len(cuts)))
        level = level * jnp.repeat(heights, dims[dim] // parts).reshape([-1 if axis == dim else 1 for axis in range(len(dims))])
    return level


def assign_block(rng, own, number, rows, number_of, top, reach, skew):
    order = jax.random.permutation(rng, number_of)
    packed, ordinary = load_shares(number_of, rows * top, reach, skew, True), load_shares(number_of, rows * top, reach, skew, False)
    places = jnp.arange(number_of)

    def named(lengths, rotation):
        used = int((lengths > 0).sum())
        fixed = max(1, used // 4)
        passed = fixed + (places - fixed + rotation * (used - fixed)) % max(1, number_of - fixed)
        return jnp.zeros((number_of,), jnp.int32).at[order[jnp.where(places < fixed, places, passed)]].set(jnp.asarray(lengths, jnp.int32))

    lengths = jnp.where(number % 4 == 0, named(packed, number // 4), named(ordinary, number - number // 4 - 1))
    mixed = jax.random.permutation(jax.random.fold_in(own, 3), number_of)
    giver, taker = mixed[0:number_of // 2 * 2:2], mixed[1:number_of // 2 * 2:2]
    margin = jnp.minimum(lengths[giver] - 1, reach - lengths[taker]) // 2
    margin = jnp.where((giver == order[0]) | (taker == order[0]) | (lengths[taker] == 0), 0, jnp.maximum(margin, 0))
    passed = jax.random.randint(jax.random.fold_in(own, 4), (number_of // 2,), 0, 1 << 20) % (margin + 1)
    lengths = lengths.at[giver].add(-passed).at[taker].add(passed)
    items = jnp.searchsorted(jnp.cumsum(lengths), jnp.arange(rows * top), side="right").astype(jnp.int32)
    listing = items.reshape(top, rows).T
    listing = listing[jax.random.permutation(jax.random.fold_in(own, 1), rows)]
    rotation = jax.random.randint(jax.random.fold_in(own, 2), (rows, 1), 0, top)
    return jnp.take_along_axis(listing, (jnp.arange(top)[None, :] + rotation) % top, axis=1)


def load_shares(amount, total, reach, skew, full):
    portions = [(1 << 20) // math.isqrt(standing ** skew) + 1 for standing in range(1, amount + 1)]
    largest = reach if full else min(reach, max(-(-total // amount), total * portions[0] // sum(portions)))
    least = 1 if total - largest >= amount - 1 else 0
    given, rest = [largest] + [least] * (amount - 1), total - largest - least * (amount - 1)
    while rest > 0:
        candidates = [i for i in range(1, amount) if given[i] < largest] or [i for i in range(1, amount) if given[i] < reach]
        mass, budget = sum([portions[i] for i in candidates]), rest
        for i in candidates:
            more = min(reach - given[i], max(1, budget * portions[i] // mass), rest)
            given[i] = given[i] + more
            rest = rest - more
    return np.array(given)


def gaussian(key, dims, deviation, bound, cuts=(), kind=jnp.bfloat16):
    result = deviation * jax.random.normal(key, dims, jnp.float32)
    if cuts:
        result = result * levels(key, dims, cuts, -0.22, 0.18)
    return jnp.clip(result, -bound, bound).astype(kind)


def setup_inputs(seed: int = 0) -> dict:
    keys = jax.random.split(jax.random.key(seed), 18)
    residual_in = gaussian(keys[0], (TOKENS, D), 1.0, 6.0, ((0, 32), (1, 16)))
    query_wide = gaussian(keys[1], (TOKENS, PAIRS * DKW), 1.0, 6.0, ((0, 32), (1, 16)))
    narrow_head_query = gaussian(keys[2], (TOKENS, PAIRS * DKN), 1.0, 6.0, ((0, 32), (1, 16)))
    forget_wide = draw_forget_wide(jax.random.fold_in(keys[17], 71), 0)
    forget_narrow = draw_forget_narrow(jax.random.fold_in(keys[17], 71), 0)
    room_wide = draw_room_wide(jax.random.fold_in(keys[17], 71), 0)
    room_narrow = draw_room_narrow(jax.random.fold_in(keys[17], 71), 0)
    values = gaussian(keys[7], (TOKENS, VAL), 1.0, 6.0, ((0, 32), (1, 16)))
    out_gate = gaussian(keys[8], (TOKENS, VAL), 1.0, 6.0, ((0, 32), (1, 16)))
    head_gain = jnp.clip(1.0 + 0.18 * jax.random.normal(keys[9], (VAL,), jnp.float32), 0.1, 1.9)
    w_out = gaussian(keys[10], (VAL, D), VAL ** -0.5, 0.125, ((1, 16),))
    norm_gain = jnp.clip(1.0 + 0.18 * jax.random.normal(keys[11], (D,), jnp.float32), 0.1, 1.9)
    route_ids_keys = jax.random.split(jax.random.fold_in(keys[12], 1), TOKENS // TOK_DEV)
    route_ids_turns = jax.random.permutation(jax.random.fold_in(keys[12], 3), TOKENS // TOK_DEV)
    route_ids = jax.vmap(lambda own, number: assign_block(jax.random.fold_in(keys[12], 2), own, number, TOK_DEV, EXPERTS, TOPK, CAP, 2))(route_ids_keys, route_ids_turns).reshape((TOKENS, TOPK))
    route_weight = jnp.clip(0.25 + 0.75 * jax.random.uniform(keys[13], (TOKENS, TOPK), jnp.float32) ** levels(keys[13], (TOKENS, TOPK), ((0, 32),), -0.2, 0.2), 0.25, 1.0)
    w_gate = gaussian(keys[14], (EXPERTS, D, FF), D ** -0.5, 0.125, ((0, 32), (2, 16)))
    w_up = gaussian(keys[15], (EXPERTS, D, FF), D ** -0.5, 0.125, ((0, 32), (2, 16)))
    w_down = gaussian(keys[16], (EXPERTS, FF, D), FF ** -0.5, 0.09375, ((0, 32), (1, 16)))
    return {"residual_in": residual_in, "query_wide": query_wide, "narrow_head_query": narrow_head_query, "forget_wide": forget_wide, "forget_narrow": forget_narrow, "room_wide": room_wide, "room_narrow": room_narrow, "values": values, "out_gate": out_gate, "head_gain": head_gain, "w_out": w_out, "norm_gain": norm_gain, "route_ids": route_ids, "route_weight": route_weight, "w_gate": w_gate, "w_up": w_up, "w_down": w_down}


EPS = 1e-06
TOP_PRECISION = lax.Precision.HIGHEST

def run_blocks(queries, rates, contents, log_decay, block_len, initial):
    length, head_count, key_dim = queries.shape
    value_dim = contents.shape[-1]
    span_count = length // block_len

    def to_spans(tensor):
        return tensor.reshape(span_count, block_len, head_count, tensor.shape[-1]).transpose(0, 2, 1, 3)
    span_query = to_spans(queries)
    span_rate = to_spans(rates)
    span_value = to_spans(contents)
    inside = jnp.cumsum(to_spans(log_decay), axis=2)
    middle = inside[:, :, block_len // 2 - 1:block_len // 2, :]
    ending = inside[:, :, block_len - 1:block_len, :]
    near_query = span_query * jnp.exp(inside - middle)
    near_rate = span_rate * jnp.exp(middle - inside)
    far_query = span_query * jnp.exp(inside)
    far_rate = span_rate * jnp.exp(ending - inside)
    fading = jnp.exp(ending[:, :, 0, :])
    causal = jnp.tril(jnp.ones((block_len, block_len), jnp.float32))

    def advance(running_total, slice_pieces):
        scores = jnp.einsum('htk,hsk->hts', slice_pieces[0], slice_pieces[1], precision=TOP_PRECISION) * causal
        final_output = jnp.einsum('hts,hsv->htv', scores, slice_pieces[4], precision=TOP_PRECISION)
        final_output = final_output + jnp.einsum('ncw,nws->ncs', slice_pieces[2], running_total, precision=TOP_PRECISION)
        running_total = slice_pieces[5][..., None] * running_total + jnp.einsum('jlg,jlq->jgq', slice_pieces[3], slice_pieces[4], precision=TOP_PRECISION)
        return (running_total, final_output)
    final, outputs = lax.scan(advance, initial, (near_query, near_rate, far_query, far_rate, span_value, fading))
    return (final, outputs.transpose(0, 2, 1, 3).reshape(length, head_count, value_dim))

def head_inputs(raw_query, raw_forget, room_vec, key_dim):
    length = raw_query.shape[0]
    activated = jax.nn.silu(raw_query.astype(jnp.float32)).reshape(length, -1, key_dim)
    in_rate = (room_vec * jax.nn.sigmoid(-raw_forget.astype(jnp.float32))).reshape(length, -1, key_dim)
    return (activated, in_rate, jnp.log1p(-in_rate))

def head_norm(outputs):
    return outputs * lax.rsqrt(lax.optimization_barrier(jnp.mean(outputs * outputs, axis=-1, keepdims=True)) + EPS)

def slot_positions(block_ids):
    matches = (block_ids[:, None] == jnp.arange(EXPERTS, dtype=jnp.int32)[None, :]).astype(jnp.int32)
    slot_rank = lax.optimization_barrier(jnp.sum((jnp.cumsum(matches, axis=0) - matches) * matches, axis=1))
    return block_ids * CAP + slot_rank

def slot_owners(positions):
    owners = jnp.full((EXPERTS * CAP,), TOK_DEV, jnp.int32)
    return owners.at[positions].set(jnp.arange(TOK_DEV * TOPK, dtype=jnp.int32) // TOPK)

def reference(residual_in, query_wide, narrow_head_query, forget_wide, forget_narrow, room_wide, room_narrow, values, out_gate, head_gain, w_out, norm_gain, route_ids, route_weight, w_gate, w_up, w_down):
    length = residual_in.shape[0]
    value_cols = values.astype(jnp.float32).reshape(length, PAIRS, 2, DV)
    wide_query, wide_rate, wide_log = head_inputs(query_wide, forget_wide, room_wide, DKW)
    narrow_query, narrow_rate, narrow_log = head_inputs(narrow_head_query, forget_narrow, room_narrow, DKN)
    _, wide_out = run_blocks(wide_query, wide_rate, value_cols[:, :, 0], wide_log, BLOCK, jnp.zeros((PAIRS, DKW, DV), jnp.float32))
    _, narrow_out = run_blocks(narrow_query, narrow_rate, value_cols[:, :, 1], narrow_log, BLOCK, jnp.zeros((PAIRS, DKN, DV), jnp.float32))
    normed_heads = jnp.stack([head_norm(wide_out), head_norm(narrow_out)], axis=2).reshape(length, VAL)
    mixed = (normed_heads * head_gain * jax.nn.silu(out_gate.astype(jnp.float32))).astype(jnp.bfloat16)
    projected = jnp.dot(mixed, w_out, preferred_element_type=jnp.float32)
    residual_mid = (residual_in.astype(jnp.float32) + projected).astype(jnp.bfloat16)
    mid_float = residual_mid.astype(jnp.float32)
    scale_rows = lax.rsqrt(lax.optimization_barrier(jnp.mean(mid_float * mid_float, axis=1, keepdims=True)) + EPS)
    token_rows = (mid_float * scale_rows * norm_gain).astype(jnp.bfloat16)
    block_ids = route_ids.reshape(N_SP, TOK_DEV * TOPK)
    positions = jax.vmap(slot_positions)(block_ids)
    owners = jax.vmap(slot_owners)(positions)
    block_start = (jnp.arange(N_SP, dtype=jnp.int32) * TOK_DEV)[:, None]
    global_owner = jnp.where(owners < TOK_DEV, owners + block_start, TOKENS).astype(jnp.int32)
    by_expert = global_owner.reshape(N_SP, EXPERTS, CAP).transpose(1, 0, 2).reshape(EXPERTS, N_SP * CAP)

    def one_expert(operands):
        gate_w, up_w, down_w, holder_index = operands
        rows_in = jnp.take(token_rows, holder_index, axis=0, mode='fill', fill_value=0)
        gate_proj = jnp.dot(rows_in, gate_w, preferred_element_type=jnp.float32)
        up_proj = jnp.dot(rows_in, up_w, preferred_element_type=jnp.float32)
        hidden = (jax.nn.silu(gate_proj) * up_proj).astype(jnp.bfloat16)
        return jnp.dot(hidden, down_w, preferred_element_type=jnp.float32)
    expert_out = lax.map(one_expert, (w_gate, w_up, w_down, by_expert))
    source_ids = jnp.arange(N_SP, dtype=jnp.int32)[:, None]
    flat_index = block_ids * (N_SP * CAP) + source_ids * CAP + (positions - block_ids * CAP)
    picked = jnp.take(expert_out.reshape(EXPERTS * N_SP * CAP, D), flat_index.reshape(-1).astype(jnp.int32), axis=0)
    routed = lax.optimization_barrier(jnp.sum((picked * route_weight.reshape(-1, 1)).reshape(TOKENS, TOPK, D), axis=1))
    return (mid_float + routed).astype(jnp.bfloat16)
```

```python
import functools

import jax
import jax.numpy as jnp
from jax import lax
from jax.experimental import pallas as pl
from jax.experimental.pallas import tpu as pltpu
from jax.sharding import PartitionSpec as P

D = 2048
DKW = 128
DKN = 64
DV = 64
EPS = 1e-06
CAP = 10
PADCAP = 16
F32 = jnp.float32
BF16 = jnp.bfloat16
TOP = lax.Precision.HIGHEST
MESH = pl.DeviceIdType.MESH


def dot(a, b, dims=((1,), (0,)), precision=None):
    return lax.dot_general(a, b, (dims, ((), ())), precision=precision, preferred_element_type=F32)


def silu(v):
    return v / (1.0 + jnp.exp(-v))


def iota(shape, dim):
    return lax.broadcasted_iota(jnp.int32, shape, dim)


def kernel(
    n_sp, n_tp, slots,
    res, qw, qn, fw, fn, room_w, room_n, val, gate_in, gain_h, w_out, gain_n, ids, rw, w_gate, w_up, w_down,
    out,
    wo_v, wg_v, wu_v, wd_v, w_sem,
    st, st_in, lg, lg_in, d2d_send, d2d_recv,
    t_src, t_buf, l_src, l_buf, t_send, t_recv, l_send, l_recv,
    x_src, x_in,
    mix, mix_send, mix_recv,
    gains, gain_send, gain_recv,
    disp_src, disp, disp_send, disp_recv,
    rows, rows_send, rows_recv,
    scat_src, scat, scat_send, scat_recv,
    ret_src, ret, ret_send, ret_recv,
    acc_g, acc_u,
):
    b = lax.axis_index("sp")
    p = lax.axis_index("tp")
    z = lax.div(b, 2)
    c = lax.rem(b, 2)
    chips = n_sp // 2
    partner = 2 * z + (1 - c)
    tokens = res.shape[0]
    padded = n_sp * PADCAP

    barrier = pltpu.get_barrier_semaphore()

    def greet_sp(i, _):
        pl.semaphore_signal(barrier, inc=1, device_id={"sp": lax.rem(b + i, n_sp)}, device_id_type=MESH)
        return 0

    def greet_tp(i, _):
        pl.semaphore_signal(barrier, inc=1, device_id={"tp": lax.rem(p + i, n_tp)}, device_id_type=MESH)
        return 0

    lax.fori_loop(1, n_sp, greet_sp, 0)
    lax.fori_loop(1, n_tp, greet_tp, 0)

    loads = [
        pltpu.make_async_copy(w_out, wo_v, w_sem.at[0]),
        pltpu.make_async_copy(w_gate.at[0], wg_v, w_sem.at[1]),
        pltpu.make_async_copy(w_up.at[0], wu_v, w_sem.at[2]),
        pltpu.make_async_copy(w_down.at[0], wd_v, w_sem.at[3]),
    ]
    for load in loads:
        load.start()

    def to_sp(src, dst, send, recv, who):
        return pltpu.make_async_remote_copy(src, dst, send, recv, device_id={"sp": who}, device_id_type=MESH)

    def to_tp(src, dst, send, recv, who):
        return pltpu.make_async_remote_copy(src, dst, send, recv, device_id={"tp": who}, device_id_type=MESH)

    low = (iota((tokens, tokens), 0) >= iota((tokens, tokens), 1)).astype(F32)

    def head(q_ref, f_ref, room_ref):
        q = silu(q_ref[...].astype(F32))
        rate = room_ref[...] / (1.0 + jnp.exp(f_ref[...].astype(F32)))
        cum = dot(low, jnp.log1p(-rate), precision=TOP)
        mid = cum[tokens // 2 - 1 : tokens // 2, :]
        end = cum[tokens - 1 : tokens, :]
        return q * jnp.exp(cum - mid), rate * jnp.exp(mid - cum), q * jnp.exp(cum), rate * jnp.exp(end - cum), end

    near_qw, near_rw, far_qw, far_rw, end_w = head(qw, fw, room_w)
    near_qn, near_rn, far_qn, far_rn, end_n = head(qn, fn, room_n)
    v = val[...].astype(F32)
    v_t = v.T
    s_w = dot(v_t[:DV], far_rw, precision=TOP)
    s_n = dot(v_t[DV:], far_rn, precision=TOP)
    s_n = jnp.concatenate([s_n[: DV // 2], s_n[DV // 2 :]], axis=1)
    st[0] = s_w[:48]
    st[1] = jnp.concatenate([s_w[48:], s_n], axis=0)
    lg[...] = jnp.concatenate([end_w, jnp.concatenate([end_n, end_n], axis=1)], axis=0)

    pl.semaphore_wait(barrier, n_sp + n_tp - 2)

    st_copy = to_sp(st.at[1 - c], st_in, d2d_send.at[0], d2d_recv.at[0], partner)
    lg_copy = to_sp(lg, lg_in, d2d_send.at[1], d2d_recv.at[1], partner)
    st_copy.start()
    lg_copy.start()

    gains[p] = jnp.broadcast_to(gain_n[...], gains.shape[1:])

    def send_gain(i, _):
        who = lax.rem(p + i, n_tp)
        to_tp(gains.at[p], gains.at[p], gain_send.at[i], gain_recv.at[p], who).start()
        return 0

    lax.fori_loop(1, n_tp, send_gain, 0)

    own_rows = iota((48, 128), 0) + 48 * c < DV

    def decay(logs):
        return jnp.exp(jnp.where(own_rows, logs[0:1], logs[1:2]))

    st_copy.wait_recv()
    lg_copy.wait_recv()
    own, other = st[c], st_in[...]
    own_log, other_log = lg[...], lg_in[...]
    first = c == 0
    even, odd = jnp.where(first, own, other), jnp.where(first, other, own)
    even_log = jnp.where(first, own_log, other_log)
    odd_log = jnp.where(first, other_log, own_log)
    t_src[...] = (decay(odd_log) * even + odd).astype(BF16)
    l_src[...] = even_log + odd_log

    def t_copy(i):
        return to_sp(t_src, t_buf.at[z], t_send.at[i], t_recv.at[z], 2 * i + c)

    def l_copy(i):
        return to_sp(l_src, l_buf.at[z], l_send.at[i], l_recv.at[z], 2 * i + c)

    def send_state(i, _):
        l_copy(i).start()
        t_copy(i).start()
        return 0

    lax.fori_loop(z + 1, chips, send_state, 0)

    def inside(near_q, near_r, content):
        scores = dot(near_q, near_r, ((1,), (1,)), precision=TOP) * low
        return dot(scores, content, precision=TOP)

    out_w = inside(near_qw, near_rw, v[:, :DV])
    out_n = inside(near_qn, near_rn, v[:, DV:])
    gated = gain_h[...] * silu(gate_in[...].astype(F32))

    lane = iota((tokens, n_sp), 1)
    hit0 = (lane == ids[:, 0:1]).astype(F32)
    hit1 = (lane == ids[:, 1:2]).astype(F32)
    strict = (iota((tokens, tokens), 0) > iota((tokens, tokens), 1)).astype(F32)
    taken = dot(strict.astype(BF16), (hit0 + hit1).astype(BF16))
    rank0 = jnp.sum(taken * hit0, axis=1, keepdims=True)
    rank1 = jnp.sum((taken + hit0) * hit1, axis=1, keepdims=True)
    pos0 = ids[:, 0:1].astype(F32) * PADCAP + rank0
    pos1 = ids[:, 1:2].astype(F32) * PADCAP + rank1
    row0 = jnp.broadcast_to(pos0, (tokens, tokens)).T[0:1]
    row1 = jnp.broadcast_to(pos1, (tokens, tokens)).T[0:1]
    slot = iota((padded, tokens), 0).astype(F32)
    pick = ((slot == row0) | (slot == row1)).astype(BF16)
    column = iota((tokens, padded), 1).astype(F32)
    weigh = jnp.where(column == pos0, rw[:, 0:1], 0.0) + jnp.where(column == pos1, rw[:, 1:2], 0.0)
    weigh_hi = weigh.astype(BF16)
    weigh_lo = (weigh - weigh_hi.astype(F32)).astype(BF16)
    filled = iota((slots, padded), 0).astype(F32)
    filled = filled + (PADCAP - CAP) * jnp.floor((filled + 0.5) * (1.0 / CAP))
    squeeze = (filled == iota((slots, padded), 1).astype(F32)).astype(BF16)
    spread = iota((padded, slots), 1).astype(F32)
    spread = spread + (PADCAP - CAP) * jnp.floor((spread + 0.5) * (1.0 / CAP))
    spread = (spread == iota((padded, slots), 0).astype(F32)).astype(BF16)

    def fold(i, carry):
        to_sp(l_src, l_buf.at[i], l_send.at[i], l_recv.at[i], partner).wait_recv()
        to_sp(t_src, t_buf.at[i], t_send.at[i], t_recv.at[i], partner).wait_recv()
        return decay(l_buf[i]) * carry + t_buf[i].astype(F32)

    in_even = lax.fori_loop(0, z, fold, jnp.zeros((48, 128), F32))
    in_odd = decay(even_log) * in_even + even
    x_src[...] = jnp.where(first, in_odd, in_even)
    x_copy = to_sp(x_src, x_in, d2d_send.at[2], d2d_recv.at[2], partner)
    x_copy.start()
    x_copy.wait_recv()
    half_own, half_other = jnp.where(first, in_even, in_odd), x_in[...]
    half0, half1 = jnp.where(first, half_own, half_other), jnp.where(first, half_other, half_own)
    in_w = jnp.concatenate([half0, half1[:16]], axis=0)
    in_n = half1[16:]
    in_n = jnp.concatenate([in_n[:, :DKN], in_n[:, DKN:]], axis=0)
    out_w = out_w + dot(far_qw, in_w, ((1,), (1,)), precision=TOP)
    out_n = out_n + dot(far_qn, in_n, ((1,), (1,)), precision=TOP)

    def normed(o):
        return o * lax.rsqrt(jnp.mean(o * o, axis=1, keepdims=True) + EPS)

    mix[p] = (jnp.concatenate([normed(out_w), normed(out_n)], axis=1) * gated).astype(BF16)

    def send_mix(i, _):
        to_tp(mix.at[p], mix.at[p], mix_send.at[i], mix_recv.at[p], lax.rem(p + i, n_tp)).start()
        return 0

    lax.fori_loop(1, n_tp, send_mix, 0)
    loads[0].wait()

    def w_out_rows(s):
        return wo_v[pl.ds(pl.multiple_of(s * 128, 128), 128), :]

    def project(i, total):
        s = lax.rem(p + n_tp - i, n_tp)
        to_tp(mix.at[s], mix.at[s], mix_send.at[i], mix_recv.at[s], s).wait_recv()
        return total + dot(mix[s], w_out_rows(s))

    projected = lax.fori_loop(1, n_tp, project, dot(mix[p], w_out_rows(p)))
    mid = (res[...].astype(F32) + projected).astype(BF16)

    packed = dot(pick, mid).astype(BF16)
    disp_src[...] = packed.reshape(n_sp, PADCAP, 128)
    disp[b] = disp_src[b]

    def send_rows(i, _):
        who = lax.rem(b + i, n_sp)
        to_sp(disp_src.at[who], disp.at[b], disp_send.at[i], disp_recv.at[b], who).start()
        return 0

    lax.fori_loop(1, n_sp, send_rows, 0)

    def have_rows(i, _):
        s = lax.rem(b + i, n_sp)
        to_sp(disp_src.at[s], disp.at[s], disp_send.at[i], disp_recv.at[s], s).wait_recv()
        return 0

    lax.fori_loop(1, n_sp, have_rows, 0)
    rows[p] = dot(squeeze, disp[...].reshape(padded, 128)).astype(BF16)

    def spread_rows(i, _):
        to_tp(rows.at[p], rows.at[p], rows_send.at[i], rows_recv.at[p], lax.rem(p + i, n_tp)).start()
        return 0

    lax.fori_loop(1, n_tp, spread_rows, 0)

    def have_gain(i, _):
        s = lax.rem(p + i, n_tp)
        to_tp(gains.at[s], gains.at[s], gain_send.at[i], gain_recv.at[s], s).wait_recv()
        return 0

    lax.fori_loop(1, n_tp, have_gain, 0)
    for load in loads[1:]:
        load.wait()
    acc_g[...] = jnp.zeros_like(acc_g)
    acc_u[...] = jnp.zeros_like(acc_u)

    def gate_up(s, squares):
        x = rows[s].astype(F32)
        y = (x * gains[s][0:1]).astype(BF16)
        at = pl.ds(pl.multiple_of(s * 128, 128), 128)
        acc_g[...] += dot(y, wg_v[at, :])
        acc_u[...] += dot(y, wu_v[at, :])
        return squares + x * x

    def gate_up_from(i, squares):
        s = lax.rem(p + n_tp - i, n_tp)
        to_tp(rows.at[s], rows.at[s], rows_send.at[i], rows_recv.at[s], s).wait_recv()
        return gate_up(s, squares)

    squares = lax.fori_loop(1, n_tp, gate_up_from, gate_up(p, jnp.zeros((slots, 128), F32)))
    scale = lax.rsqrt(jnp.sum(squares, axis=1, keepdims=True) * (1.0 / D) + EPS)
    hidden = (silu(acc_g[...] * scale) * (acc_u[...] * scale)).astype(BF16)

    def down(j):
        return dot(hidden, wd_v[:, pl.ds(pl.multiple_of(j * 128, 128), 128)])

    def send_part(i, _):
        who = lax.rem(p + i, n_tp)
        scat_src[who] = down(who).astype(BF16)
        to_tp(scat_src.at[who], scat.at[p], scat_send.at[i], scat_recv.at[p], who).start()
        return 0

    lax.fori_loop(1, n_tp, send_part, 0)

    def add_part(i, total):
        s = lax.rem(p + n_tp - i, n_tp)
        to_tp(scat_src.at[s], scat.at[s], scat_send.at[i], scat_recv.at[s], s).wait_recv()
        return total + scat[s].astype(F32)

    total = lax.fori_loop(1, n_tp, add_part, down(p)).astype(BF16)

    ret_src[...] = dot(spread, total).astype(BF16).reshape(n_sp, PADCAP, 128)
    ret[b] = ret_src[b]

    def send_back(i, _):
        who = lax.rem(b + i, n_sp)
        to_sp(ret_src.at[who], ret.at[b], ret_send.at[i], ret_recv.at[b], who).start()
        return 0

    lax.fori_loop(1, n_sp, send_back, 0)

    def have_back(i, _):
        s = lax.rem(b + i, n_sp)
        to_sp(ret_src.at[s], ret.at[s], ret_send.at[i], ret_recv.at[s], s).wait_recv()
        return 0

    lax.fori_loop(1, n_sp, have_back, 0)
    back = ret[...].reshape(padded, 128)
    moe = dot(weigh_hi, back) + dot(weigh_lo, back)
    out[...] = (mid.astype(F32) + moe).astype(BF16)

    st_copy.wait_send()
    lg_copy.wait_send()
    x_copy.wait_send()

    def state_gone(i, _):
        t_copy(i).wait_send()
        l_copy(i).wait_send()
        return 0

    lax.fori_loop(z + 1, chips, state_gone, 0)

    def tp_gone(i, _):
        who = lax.rem(p + i, n_tp)
        to_tp(gains.at[p], gains.at[p], gain_send.at[i], gain_recv.at[p], who).wait_send()
        to_tp(mix.at[p], mix.at[p], mix_send.at[i], mix_recv.at[p], who).wait_send()
        to_tp(rows.at[p], rows.at[p], rows_send.at[i], rows_recv.at[p], who).wait_send()
        to_tp(scat_src.at[who], scat.at[p], scat_send.at[i], scat_recv.at[p], who).wait_send()
        return 0

    lax.fori_loop(1, n_tp, tp_gone, 0)

    def sp_gone(i, _):
        who = lax.rem(b + i, n_sp)
        to_sp(disp_src.at[who], disp.at[b], disp_send.at[i], disp_recv.at[b], who).wait_send()
        to_sp(ret_src.at[who], ret.at[b], ret_send.at[i], ret_recv.at[b], who).wait_send()
        return 0

    lax.fori_loop(1, n_sp, sp_gone, 0)


def body(n_sp, n_tp, *args):
    (res, qw, qn, fw, fn, room_w, room_n, val, gate_in, gain_h, w_out, gain_n, ids, rw, w_gate, w_up, w_down) = args
    tokens = res.shape[0]
    hidden = w_gate.shape[2]
    chips = n_sp // 2
    slots = n_sp * CAP
    row = lambda a: a.reshape(1, -1)
    vmem = pl.BlockSpec(memory_space=pltpu.VMEM)
    hbm = pl.BlockSpec(memory_space=pl.ANY)
    dma = pltpu.SemaphoreType.DMA
    V = pltpu.VMEM
    scratch = [
        V((D, 128), BF16), V((D, hidden), BF16), V((D, hidden), BF16), V((hidden, D), BF16), dma((4,)),
        V((2, 48, 128), F32), V((48, 128), F32), V((2, 128), F32), V((2, 128), F32), dma((3,)), dma((3,)),
        V((48, 128), BF16), V((chips, 48, 128), BF16), V((2, 128), F32), V((chips, 2, 128), F32),
        dma((chips,)), dma((chips,)), dma((chips,)), dma((chips,)),
        V((48, 128), F32), V((48, 128), F32),
        V((n_tp, tokens, 128), BF16), dma((n_tp,)), dma((n_tp,)),
        V((n_tp, 8, 128), F32), dma((n_tp,)), dma((n_tp,)),
        V((n_sp, PADCAP, 128), BF16), V((n_sp, PADCAP, 128), BF16), dma((n_sp,)), dma((n_sp,)),
        V((n_tp, slots, 128), BF16), dma((n_tp,)), dma((n_tp,)),
        V((n_tp, slots, 128), BF16), V((n_tp, slots, 128), BF16), dma((n_tp,)), dma((n_tp,)),
        V((n_sp, PADCAP, 128), BF16), V((n_sp, PADCAP, 128), BF16), dma((n_sp,)), dma((n_sp,)),
        V((slots, hidden), F32), V((slots, hidden), F32),
    ]
    return pl.pallas_call(
        functools.partial(kernel, n_sp, n_tp, slots),
        out_shape=jax.ShapeDtypeStruct((tokens, 128), BF16),
        in_specs=[vmem] * 10 + [hbm] + [vmem] * 3 + [hbm] * 3,
        out_specs=vmem,
        scratch_shapes=scratch,
        compiler_params=pltpu.CompilerParams(
            collective_id=0, has_side_effects=True, vmem_limit_bytes=48 * 1024 * 1024
        ),
    )(res, qw, qn, fw, fn, row(room_w), row(room_n), val, gate_in, row(gain_h), w_out, row(gain_n), ids, rw, w_gate, w_up, w_down)


def solution(mesh):
    both = P("sp", "tp")
    placed = (
        both, both, both, both, both, P("tp"), P("tp"), both, both, P("tp"), P(None, "tp"), P("tp"),
        P("sp", None), P("sp", None), P("sp", None, "tp"), P("sp", None, "tp"), P("sp", "tp", None),
    )
    fn = functools.partial(body, mesh.shape["sp"], mesh.shape["tp"])
    return jax.shard_map(fn, mesh=mesh, in_specs=placed, out_specs=both, check_vma=False)
```

```python
import functools

import jax
import jax.numpy as jnp
from jax import lax
from jax.experimental import pallas as pl
from jax.experimental.pallas import tpu as pltpu
from jax.sharding import PartitionSpec as P

D = 2048
DKW = 128
DKN = 64
DV = 64
EPS = 1e-06
CAP = 10
PADCAP = 16
NODE = 4
PART = (DV + DV // 2) // NODE
F32 = jnp.float32
BF16 = jnp.bfloat16
TOP = lax.Precision.HIGHEST
MESH = pl.DeviceIdType.MESH


PROFILE = False
scope = []


def mark(name=None):
    if PROFILE:
        while scope:
            scope.pop().__exit__(None, None, None)
        if name:
            scope.append(jax.named_scope(name))
            scope[-1].__enter__()


def dot(a, b, dims=((1,), (0,)), precision=None):
    return lax.dot_general(a, b, (dims, ((), ())), precision=precision, preferred_element_type=F32)


def silu(v):
    return v / (1.0 + jnp.exp(-v))


def iota(shape, dim):
    return lax.broadcasted_iota(jnp.int32, shape, dim)


def kernel(
    n_sp, n_tp, slots,
    res_h, qw_h, qn_h, fw_h, fn_h, room_w_h, room_n_h, val_h, gate_h, gain_h_h, w_out, gain_n_h, ids_h, rw_h,
    w_gate, w_up, w_down,
    out,
    res, qw, qn, fw, fn, room_w, room_n, val, gate_in, gain_h, gain_n, ids, rw, in_sem,
    wo_v, wgu, wd_v, w_sem,
    st, st_in, st_send, st_recv, lg, lg_send, lg_recv,
    t_src, t_buf, l_src, l_buf, t_send, t_recv, l_send, l_recv,
    x_src, x_in, x_send, x_recv,
    mix, mix_send, mix_recv,
    gains, gain_send, gain_recv,
    disp_src, disp, disp_send, disp_recv,
    rows, rows_send, rows_recv,
    heavy_src, heavy, heavy_send, heavy_recv,
    light_src, light, light_send, light_recv,
    keep, line,
    ret_src, ret, ret_send, ret_recv,
    acc, squares,
):
    b = lax.axis_index("sp")
    p = lax.axis_index("tp")
    nodes = n_sp // NODE
    node, q = lax.div(b, NODE), lax.rem(b, NODE)
    tokens = res.shape[0]
    padded = n_sp * PADCAP

    small = (
        (qw_h, qw), (fw_h, fw), (qn_h, qn), (fn_h, fn), (room_w_h, room_w), (room_n_h, room_n), (val_h, val),
        (gate_h, gate_in), (gain_h_h, gain_h), (gain_n_h, gain_n), (ids_h, ids), (rw_h, rw), (res_h, res),
    )
    small = [pltpu.make_async_copy(src, dst, in_sem.at[k]) for k, (src, dst) in enumerate(small)]
    hidden_units = w_down.shape[1]
    loads = [
        pltpu.make_async_copy(w_out, wo_v, w_sem.at[0]),
        pltpu.make_async_copy(w_gate.at[0], wgu.at[:, pl.ds(0, hidden_units)], w_sem.at[1]),
        pltpu.make_async_copy(w_up.at[0], wgu.at[:, pl.ds(hidden_units, hidden_units)], w_sem.at[2]),
    ]
    for k in range(n_tp):
        loads.append(pltpu.make_async_copy(w_down.at[0, :, pl.ds(128 * k, 128)], wd_v.at[k], w_sem.at[3 + k]))
    for load in small:
        load.start()
    disp[...] = jnp.zeros_like(disp)
    ret[...] = jnp.zeros_like(ret)

    barrier = pltpu.get_barrier_semaphore()

    def greet_sp(i, _):
        pl.semaphore_signal(barrier, inc=1, device_id={"sp": lax.rem(b + i, n_sp)}, device_id_type=MESH)
        return 0

    def greet_tp(i, _):
        pl.semaphore_signal(barrier, inc=1, device_id={"tp": lax.rem(p + i, n_tp)}, device_id_type=MESH)
        return 0

    lax.fori_loop(1, n_sp, greet_sp, 0)
    lax.fori_loop(1, n_tp, greet_tp, 0)
    for load in loads:
        load.start()
    for load in small:
        load.wait()

    def to_sp(src, dst, send, recv, who):
        return pltpu.make_async_remote_copy(src, dst, send, recv, device_id={"sp": who}, device_id_type=MESH)

    def to_tp(src, dst, send, recv, who):
        return pltpu.make_async_remote_copy(src, dst, send, recv, device_id={"tp": who}, device_id_type=MESH)

    mark("local")
    low = (iota((tokens, tokens), 0) >= iota((tokens, tokens), 1)).astype(F32)

    def head(q, f, room_ref):
        q = silu(q)
        rate = room_ref[...] / (1.0 + jnp.exp(f))
        cum = dot(low, jnp.log1p(-rate), precision=TOP)
        mid = cum[tokens // 2 - 1 : tokens // 2, :]
        end = cum[tokens - 1 : tokens, :]
        return q * jnp.exp(cum - mid), rate * jnp.exp(mid - cum), q * jnp.exp(cum), rate * jnp.exp(end - cum), end

    near_qw, near_rw, far_qw, far_rw, end_w = head(qw[...].astype(F32), fw[...].astype(F32), room_w)
    near_qn, near_rn, far_qn, far_rn, end_n = head(qn[...].astype(F32).T, fn[...].astype(F32).T, room_n)
    v = val[...].astype(F32)
    v_t = v.T
    s_w = dot(v_t[:DV], far_rw, precision=TOP)
    s_n = dot(v_t[DV:], far_rn, precision=TOP)
    s_n = jnp.concatenate([s_n[: DV // 2], s_n[DV // 2 :]], axis=1)
    states = jnp.concatenate([s_w, s_n], axis=0)
    for j in range(NODE):
        st[j] = states[j * PART : (j + 1) * PART]
    lg[q] = jnp.concatenate([end_w, jnp.concatenate([end_n, end_n], axis=1)], axis=0)

    mark("barrier")
    pl.semaphore_wait(barrier, n_sp + n_tp - 2)

    mark("d2d")
    def mate(i):
        return lax.rem(q + i, NODE)

    def st_copy(i, who, slot):
        return to_sp(st.at[who], st_in.at[slot], st_send.at[i], st_recv.at[slot], NODE * node + who)

    def lg_copy(i, who, slot):
        return to_sp(lg.at[slot], lg.at[slot], lg_send.at[i], lg_recv.at[slot], NODE * node + who)

    def x_copy(i, who, slot):
        return to_sp(x_src.at[who], x_in.at[slot], x_send.at[i], x_recv.at[slot], NODE * node + who)

    for i in range(1, NODE):
        lg_copy(i, mate(i), q).start()
        st_copy(i, mate(i), q).start()
    st_in[q] = st[q]

    gains[p] = jnp.broadcast_to(gain_n[...], gains.shape[1:])

    def send_gain(i, _):
        who = lax.rem(p + i, n_tp)
        to_tp(gains.at[p], gains.at[p], gain_send.at[i], gain_recv.at[p], who).start()
        return 0

    lax.fori_loop(1, n_tp, send_gain, 0)

    own_rows = iota((PART, 128), 0) + PART * q < DV

    def decay(logs):
        return jnp.exp(jnp.where(own_rows, logs[0:1], logs[1:2]))

    mark("d2dwait")
    for i in range(1, NODE):
        lg_copy(i, mate(i), mate(i)).wait_recv()
        st_copy(i, mate(i), mate(i)).wait_recv()
    decays = [decay(lg[j]) for j in range(NODE)]
    whole = st_in[0]
    for j in range(1, NODE):
        whole = decays[j] * whole + st_in[j]
    t_src[...] = whole.astype(BF16)
    l_src[...] = (lg[0] + lg[1]) + (lg[2] + lg[3])

    def t_copy(i, slot):
        return to_sp(t_src, t_buf.at[slot], t_send.at[i], t_recv.at[slot], NODE * i + q)

    def l_copy(i, slot):
        return to_sp(l_src, l_buf.at[slot], l_send.at[i], l_recv.at[slot], NODE * i + q)

    def send_state(i, _):
        l_copy(i, node).start()
        t_copy(i, node).start()
        return 0

    lax.fori_loop(node + 1, nodes, send_state, 0)

    mark("inner")
    def inside(near_q, near_r, content):
        scores = dot(near_q, near_r, ((1,), (1,)), precision=TOP) * low
        return dot(scores, content, precision=TOP)

    out_w = inside(near_qw, near_rw, v[:, :DV])
    out_n = inside(near_qn, near_rn, v[:, DV:])
    gated = gain_h[...] * silu(gate_in[...].astype(F32))

    sub = iota((n_sp, tokens), 0)
    hit0 = (sub == ids[0:1, :]).astype(F32)
    hit1 = (sub == ids[1:2, :]).astype(F32)
    strict = (iota((tokens, tokens), 0) < iota((tokens, tokens), 1)).astype(BF16)
    taken = dot((hit0 + hit1).astype(BF16), strict)
    row0 = ids[0:1, :].astype(F32) * PADCAP + jnp.sum(taken * hit0, axis=0, keepdims=True)
    row1 = ids[1:2, :].astype(F32) * PADCAP + jnp.sum((taken + hit0) * hit1, axis=0, keepdims=True)

    def upright(row):
        return jnp.broadcast_to(row, (tokens, tokens)).T[:, 0:1]

    pos0, pos1, weight0, weight1 = upright(row0), upright(row1), upright(rw[0:1, :]), upright(rw[1:2, :])
    slot = iota((padded, tokens), 0).astype(F32)
    pick = ((slot == row0) | (slot == row1)).astype(BF16)
    column = iota((tokens, padded), 1).astype(F32)
    weigh = jnp.where(column == pos0, weight0, 0.0) + jnp.where(column == pos1, weight1, 0.0)
    weigh_hi = weigh.astype(BF16)
    weigh_lo = (weigh - weigh_hi.astype(F32)).astype(BF16)
    filled = iota((slots, padded), 0).astype(F32)
    filled = filled + (PADCAP - CAP) * jnp.floor((filled + 0.5) * (1.0 / CAP))
    squeeze = (filled == iota((slots, padded), 1).astype(F32)).astype(BF16)
    spread = iota((padded, slots), 1).astype(F32)
    spread = spread + (PADCAP - CAP) * jnp.floor((spread + 0.5) * (1.0 / CAP))
    spread = (spread == iota((padded, slots), 0).astype(F32)).astype(BF16)

    mark("fold")
    def fold(i, carry):
        l_copy(i, i).wait_recv()
        t_copy(i, i).wait_recv()
        return decay(l_buf[i]) * carry + t_buf[i].astype(F32)

    carry = lax.fori_loop(0, node, fold, jnp.zeros((PART, 128), F32))
    for j in range(NODE):
        x_src[j] = carry
        if j + 1 < NODE:
            carry = decays[j] * carry + st_in[j]
    for i in range(1, NODE):
        x_copy(i, mate(i), q).start()
    x_in[q] = x_src[q]
    mark("xwait")
    for i in range(1, NODE):
        x_copy(i, mate(i), mate(i)).wait_recv()
    mark("mix")
    before = jnp.concatenate([x_in[j] for j in range(NODE)], axis=0)
    in_w = before[:DV]
    in_n = before[DV:]
    in_n = jnp.concatenate([in_n[:, :DKN], in_n[:, DKN:]], axis=0)
    out_w = out_w + dot(far_qw, in_w, ((1,), (1,)), precision=TOP)
    out_n = out_n + dot(far_qn, in_n, ((1,), (1,)), precision=TOP)

    def normed(o):
        return o * lax.rsqrt(jnp.mean(o * o, axis=1, keepdims=True) + EPS)

    mix[p] = (jnp.concatenate([normed(out_w), normed(out_n)], axis=1) * gated).astype(BF16)

    def send_mix(i, _):
        to_tp(mix.at[p], mix.at[p], mix_send.at[i], mix_recv.at[p], lax.rem(p + i, n_tp)).start()
        return 0

    lax.fori_loop(1, n_tp, send_mix, 0)
    mark("project")
    loads[0].wait()

    def w_out_rows(s):
        return wo_v[pl.ds(pl.multiple_of(s * 128, 128), 128), :]

    def project(i, total):
        s = lax.rem(p + n_tp - i, n_tp)
        to_tp(mix.at[s], mix.at[s], mix_send.at[i], mix_recv.at[s], s).wait_recv()
        return total + dot(mix[s], w_out_rows(s))

    projected = lax.fori_loop(1, n_tp, project, dot(mix[p], w_out_rows(p)))
    mark("pack")
    mid = (res[...].astype(F32) + projected).astype(BF16)

    packed = dot(pick, mid).astype(BF16)
    disp_src[...] = packed.reshape(n_sp, PADCAP, 128)
    disp[b] = disp_src[b]

    used = pl.ds(0, CAP)

    def disp_copy(i, src, dst, who):
        return to_sp(disp_src.at[src, used], disp.at[dst, used], disp_send.at[i], disp_recv.at[dst], who)

    def ret_copy(i, src, dst, who):
        return to_sp(ret_src.at[src, used], ret.at[dst, used], ret_send.at[i], ret_recv.at[dst], who)

    def outward(i):
        step = lax.div(i + 1, 2)
        return lax.rem(n_sp // 2 + n_sp + b + step - (2 * step) * lax.rem(i, 2), n_sp)

    def send_rows(i, _):
        who = outward(i)
        disp_copy(i, who, b, who).start()
        return 0

    lax.fori_loop(0, n_sp - 1, send_rows, 0)

    def have_rows(i, _):
        s = lax.rem(b + i, n_sp)
        disp_copy(i, s, s, s).wait_recv()
        return 0

    mark("dispwait")
    lax.fori_loop(1, n_sp, have_rows, 0)
    mark("squeeze")
    rows[p] = dot(squeeze, disp[...].reshape(padded, 128)).astype(BF16)

    side = 4
    half, part = slots // 2, slots // 4
    x, y = lax.rem(p, side), lax.div(p, side)
    spots = ((x, y), (y, x))
    sent = []

    def near(v, step):
        return lax.rem(v + side + step, side)

    def place(plan, f, s):
        return s * side + f if plan == 0 else f * side + s

    def piece(plan, src, which):
        start, size = {"all": (0, half), "lo": (0, part), "hi": (part, part)}[which]
        return rows.at[src, pl.ds(plan * half + start, size)]

    def push(plan, src, which, who):
        at, k = piece(plan, src, which), sum(1 for q, _ in sent if q == plan)
        copy = to_tp(at, at, rows_send.at[plan, k], rows_recv.at[plan, src, int(which == "hi")], who)
        copy.start()
        sent.append((plan, copy))

    def arrive(plan, src, which):
        at, other = piece(plan, src, which), lax.rem(p + 1, n_tp)
        to_tp(at, at, rows_send.at[plan, 0], rows_recv.at[plan, src, int(which == "hi")], other).wait_recv()

    def gate_up(plan, src):
        at = pl.ds(plan * half, half)
        x_in_half = rows[src, at].astype(F32)
        content = (x_in_half * gains[src][0:1]).astype(BF16)
        acc[at, :] += dot(content, wgu[pl.ds(pl.multiple_of(src * 128, 128), 128), :])
        squares[at, :] += x_in_half * x_in_half

    plans = [(plan, f, s) for plan, (f, s) in enumerate(spots)]
    for plan, f, s in plans:
        for who in (place(plan, near(f, 1), s), place(plan, near(f, -1), s), place(plan, f, near(s, 1)), place(plan, f, near(s, -1))):
            push(plan, p, "all", who)
    mark("agown")

    def have_gain(i, _):
        s = lax.rem(p + i, n_tp)
        to_tp(gains.at[s], gains.at[s], gain_send.at[i], gain_recv.at[s], s).wait_recv()
        return 0

    lax.fori_loop(1, n_tp, have_gain, 0)
    for load in loads[1:]:
        load.wait()
    acc[...] = jnp.zeros_like(acc)
    squares[...] = jnp.zeros_like(squares)
    for plan, f, s in plans:
        gate_up(plan, p)
    mark("ag1")
    for plan, f, s in plans:
        for step, which in ((-1, "lo"), (1, "hi")):
            src = place(plan, near(f, step), s)
            arrive(plan, src, "all")
            push(plan, src, which, place(plan, near(f, -step), s))
            push(plan, src, "all", place(plan, f, near(s, 1)))
            push(plan, src, "all", place(plan, f, near(s, -1)))
    mark("ag2")

    def pass_on(plan, f, f_from, s):
        for step, which in ((-1, "lo"), (1, "hi")):
            src = place(plan, f_from, near(s, step))
            arrive(plan, src, "all")
            push(plan, src, which, place(plan, f, near(s, -step)))

    def use(plan, f_from, s_from):
        gate_up(plan, place(plan, f_from, s_from))

    for plan, f, s in plans:
        pass_on(plan, f, f, s)
    for plan, f, s in plans:
        for step in (-1, 1):
            use(plan, near(f, step), s)
    mark("ag3")
    for plan, f, s in plans:
        src = place(plan, near(f, 2), s)
        arrive(plan, src, "lo")
        arrive(plan, src, "hi")
        push(plan, src, "all", place(plan, f, near(s, 1)))
        push(plan, src, "all", place(plan, f, near(s, -1)))
    for plan, f, s in plans:
        for step in (-1, 1):
            use(plan, f, near(s, step))
    mark("ag4")
    for plan, f, s in plans:
        pass_on(plan, f, near(f, -1), s)
        pass_on(plan, f, near(f, 1), s)
    for plan, f, s in plans:
        use(plan, near(f, 2), s)
        for step in (-1, 1):
            use(plan, near(f, -1), near(s, step))
    mark("ag5")
    for plan, f, s in plans:
        pass_on(plan, f, near(f, 2), s)
    for plan, f, s in plans:
        for step in (-1, 1):
            use(plan, near(f, 1), near(s, step))
            use(plan, near(f, 2), near(s, step))
    mark("ag6")
    for step in (0, -1, 1, 2):
        for plan, f, s in plans:
            src = place(plan, near(f, step), near(s, 2))
            arrive(plan, src, "lo")
            arrive(plan, src, "hi")
            gate_up(plan, src)
    mark("act")
    scale = lax.rsqrt(jnp.sum(squares[...], axis=1, keepdims=True) * (1.0 / D) + EPS)
    hidden = (silu(acc[:, :hidden_units] * scale) * (acc[:, hidden_units:] * scale)).astype(BF16)
    mark("down")

    def partial(plan, f, s):
        right = jnp.concatenate([wd_v[place(plan, f, k)] for k in range(side)], axis=1)
        return dot(hidden[plan * half : (plan + 1) * half], right)

    def blocks(value):
        return [[value[q * part : (q + 1) * part, 128 * k : 128 * k + 128] for k in range(side)] for q in range(2)]

    def heavy_copy(plan, way, kind, who):
        return to_tp(
            heavy_src.at[plan, way, kind], heavy.at[plan, way, kind],
            heavy_send.at[plan, way, kind], heavy_recv.at[plan, way, kind], who,
        )

    def light_copy(plan, f, s, step):
        at = plan, step - 1
        return to_tp(
            light_src.at[at], light.at[at], light_send.at[at], light_recv.at[at], place(plan, f, near(s, step)),
        )

    ways = ((0, 1), (1, -1))
    for plan, f, s in plans:
        far = blocks(partial(plan, near(f, 2), s))
        for way, step in ways:
            for k in range(side):
                heavy_src[plan, way, 0, k] = far[way][k].astype(BF16)
            heavy_copy(plan, way, 0, place(plan, near(f, step), s)).start()
    for plan, f, s in plans:
        for way, step in ways:
            next_to = blocks(partial(plan, near(f, step), s))
            for k in range(side):
                heavy_src[plan, way, 1, k] = next_to[1 - way][k].astype(BF16)
                keep[plan, way, k] = next_to[way][k]
            heavy_copy(plan, way, 1, place(plan, near(f, step), s)).start()
    for plan, f, s in plans:
        own = blocks(partial(plan, f, s))
        for q in range(2):
            for k in range(side):
                line[plan, q, k] = own[q][k]
    mark("rs1")
    for plan, f, s in plans:
        for way, step in ways:
            heavy_copy(plan, way, 0, place(plan, near(f, step), s)).wait_recv()
            heavy_src[plan, way, 2] = (keep[plan, way] + heavy[plan, way, 0].astype(F32)).astype(BF16)
            heavy_copy(plan, way, 2, place(plan, near(f, step), s)).start()
    mark("rs2")
    for plan, f, s in plans:
        for way, step in ways:
            heavy_copy(plan, way, 1, place(plan, near(f, step), s)).wait_recv()
            line[plan, 1 - way] += heavy[plan, way, 1].astype(F32)
    mark("rs3")
    for plan, f, s in plans:
        for way, step in ways:
            heavy_copy(plan, way, 2, place(plan, near(f, step), s)).wait_recv()
            line[plan, way] += heavy[plan, way, 2].astype(F32)
        for step in (2, 1, 3):
            for k in range(2):
                light_src[plan, step - 1, k] = line[plan, k, near(s, step)].astype(BF16)
            light_copy(plan, f, s, step).start()
    mark("rs4")
    sums = []
    for plan, f, s in plans:
        value = [line[plan, k, s] for k in range(2)]
        for step in (1, 3, 2):
            light_copy(plan, f, s, step).wait_recv()
            value = [value[k] + light[plan, step - 1, k].astype(F32) for k in range(2)]
        sums += value
    total = jnp.concatenate(sums, axis=0).astype(BF16)

    mark("retsend")
    ret_src[...] = dot(spread, total).astype(BF16).reshape(n_sp, PADCAP, 128)
    ret[b] = ret_src[b]

    def send_back(i, _):
        who = outward(i)
        ret_copy(i, who, b, who).start()
        return 0

    lax.fori_loop(0, n_sp - 1, send_back, 0)

    for i in range(1, NODE):
        st_copy(i, mate(i), q).wait_send()
        lg_copy(i, mate(i), q).wait_send()
        x_copy(i, mate(i), q).wait_send()

    def state_gone(i, _):
        t_copy(i, node).wait_send()
        l_copy(i, node).wait_send()
        return 0

    lax.fori_loop(node + 1, nodes, state_gone, 0)

    def tp_gone(i, _):
        who = lax.rem(p + i, n_tp)
        to_tp(gains.at[p], gains.at[p], gain_send.at[i], gain_recv.at[p], who).wait_send()
        to_tp(mix.at[p], mix.at[p], mix_send.at[i], mix_recv.at[p], who).wait_send()
        return 0

    lax.fori_loop(1, n_tp, tp_gone, 0)

    for _, copy in sent:
        copy.wait_send()
    for plan, f, s in plans:
        for way, step in ways:
            for kind in range(3):
                heavy_copy(plan, way, kind, place(plan, near(f, step), s)).wait_send()
        for step in (1, 2, 3):
            light_copy(plan, f, s, step).wait_send()

    def disp_gone(i, _):
        who = outward(i)
        disp_copy(i, who, b, who).wait_send()
        return 0

    lax.fori_loop(0, n_sp - 1, disp_gone, 0)

    def back_gone(i, _):
        who = outward(i)
        ret_copy(i, who, b, who).wait_send()
        return 0

    def have_back(i, _):
        s = lax.rem(b + i, n_sp)
        ret_copy(i, s, s, s).wait_recv()
        return 0

    mark("retwait")
    lax.fori_loop(1, n_sp, have_back, 0)
    mark("final")
    back = ret[...].reshape(padded, 128)
    moe = dot(weigh_hi, back) + dot(weigh_lo, back)
    out[...] = (mid.astype(F32) + moe).astype(BF16)

    mark("sendwait")
    lax.fori_loop(0, n_sp - 1, back_gone, 0)
    mark()


def body(n_sp, n_tp, *args):
    (res, qw, qn, fw, fn, room_w, room_n, val, gate_in, gain_h, w_out, gain_n, ids, rw, w_gate, w_up, w_down) = args
    tokens = res.shape[0]
    hidden = w_gate.shape[2]
    nodes = n_sp // NODE
    slots = n_sp * CAP
    row = lambda a: a.reshape(1, -1)
    hbm = pl.BlockSpec(memory_space=pl.ANY)
    dma = pltpu.SemaphoreType.DMA
    V = pltpu.VMEM
    half, part = slots // 2, slots // 4
    small = [res, qw, qn.T, fw, fn.T, row(room_w), row(room_n), val, gate_in, row(gain_h), row(gain_n), ids.T, rw.T]
    scratch = [
        *[V(a.shape, a.dtype) for a in small], dma((len(small),)),
        V((D, 128), BF16), V((D, 2 * hidden), BF16), V((n_tp, hidden, 128), BF16), dma((3 + n_tp,)),
        V((NODE, PART, 128), F32), V((NODE, PART, 128), F32), dma((NODE,)), dma((NODE,)),
        V((NODE, 2, 128), F32), dma((NODE,)), dma((NODE,)),
        V((PART, 128), BF16), V((nodes, PART, 128), BF16), V((2, 128), F32), V((nodes, 2, 128), F32),
        dma((nodes,)), dma((nodes,)), dma((nodes,)), dma((nodes,)),
        V((NODE, PART, 128), F32), V((NODE, PART, 128), F32), dma((NODE,)), dma((NODE,)),
        V((n_tp, tokens, 128), BF16), dma((n_tp,)), dma((n_tp,)),
        V((n_tp, 8, 128), F32), dma((n_tp,)), dma((n_tp,)),
        V((n_sp, PADCAP, 128), BF16), V((n_sp, PADCAP, 128), BF16), dma((n_sp,)), dma((n_sp,)),
        V((n_tp, slots, 128), BF16), dma((2, 20)), dma((2, n_tp, 2)),
        V((2, 2, 3, 4, part, 128), BF16), V((2, 2, 3, 4, part, 128), BF16), dma((2, 2, 3)), dma((2, 2, 3)),
        V((2, 3, 2, part, 128), BF16), V((2, 3, 2, part, 128), BF16), dma((2, 3)), dma((2, 3)),
        V((2, 2, 4, part, 128), F32), V((2, 2, 4, part, 128), F32),
        V((n_sp, PADCAP, 128), BF16), V((n_sp, PADCAP, 128), BF16), dma((n_sp,)), dma((n_sp,)),
        V((slots, 2 * hidden), F32), V((slots, 128), F32),
    ]
    return pl.pallas_call(
        functools.partial(kernel, n_sp, n_tp, slots),
        out_shape=jax.ShapeDtypeStruct((tokens, 128), BF16),
        in_specs=[hbm] * 17,
        out_specs=pl.BlockSpec(memory_space=pltpu.VMEM),
        scratch_shapes=scratch,
        compiler_params=pltpu.CompilerParams(
            collective_id=0, has_side_effects=True, vmem_limit_bytes=67043328
        ),
    )(*small[:10], w_out, *small[10:], w_gate, w_up, w_down)


def solution(mesh):
    both = P("sp", "tp")
    placed = (
        both, both, both, both, both, P("tp"), P("tp"), both, both, P("tp"), P(None, "tp"), P("tp"),
        P("sp", None), P("sp", None), P("sp", None, "tp"), P("sp", None, "tp"), P("sp", "tp", None),
    )
    fn = functools.partial(body, mesh.shape["sp"], mesh.shape["tp"])
    return jax.shard_map(fn, mesh=mesh, in_specs=placed, out_specs=both, check_vma=False)
```

```python
import functools

import jax
import jax.numpy as jnp
from jax import lax
from jax.experimental import pallas as pl
from jax.experimental.pallas import tpu as pltpu
from jax.sharding import PartitionSpec as P

D = 2048
DKW = 128
DKN = 64
DV = 64
EPS = 1e-06
CAP = 10
PADCAP = 16
NODE = 4
PART = (DV + DV // 2) // NODE
F32 = jnp.float32
BF16 = jnp.bfloat16
TOP = lax.Precision.HIGHEST
MESH = pl.DeviceIdType.MESH


PROFILE = False
scope = []


def mark(name=None):
    if PROFILE:
        while scope:
            scope.pop().__exit__(None, None, None)
        if name:
            scope.append(jax.named_scope(name))
            scope[-1].__enter__()


def dot(a, b, dims=((1,), (0,)), precision=None):
    return lax.dot_general(a, b, (dims, ((), ())), precision=precision, preferred_element_type=F32)


def silu(v):
    return v / (1.0 + jnp.exp(-v))


def iota(shape, dim):
    return lax.broadcasted_iota(jnp.int32, shape, dim)


def kernel(
    n_sp, n_tp, slots,
    res_h, qw_h, qn_h, fw_h, fn_h, room_w_h, room_n_h, val_h, gate_h, gain_h_h, w_out, gain_n_h, ids_h, rw_h,
    w_gate, w_up, w_down,
    out,
    res, qw, qn, fw, fn, room_w, room_n, val, gate_in, gain_h, gain_n, ids, rw, in_sem,
    wo_v, wgu, wd_v, w_sem,
    st, st_in, st_send, st_recv, lg, lg_send, lg_recv,
    t_src, t_buf, l_src, l_buf, t_send, t_recv, l_send, l_recv,
    x_src, x_in, x_send, x_recv,
    mix, mix_send, mix_recv,
    gains, gain_send, gain_recv,
    disp_src, disp, disp_send, disp_recv,
    rows, rows_send, rows_recv,
    heavy_src, heavy, heavy_send, heavy_recv,
    light_src, light, light_send, light_recv,
    keep, line,
    ret_src, ret, ret_send, ret_recv,
    acc, squares,
):
    b = lax.axis_index("sp")
    p = lax.axis_index("tp")
    nodes = n_sp // NODE
    node, q = lax.div(b, NODE), lax.rem(b, NODE)
    tokens = res.shape[0]
    padded = n_sp * PADCAP

    small = (
        (qw_h, qw), (fw_h, fw), (qn_h, qn), (fn_h, fn), (room_w_h, room_w), (room_n_h, room_n), (val_h, val),
        (gate_h, gate_in), (gain_h_h, gain_h), (gain_n_h, gain_n), (ids_h, ids), (rw_h, rw), (res_h, res),
    )
    small = [pltpu.make_async_copy(src, dst, in_sem.at[k]) for k, (src, dst) in enumerate(small)]
    hidden_units = w_down.shape[1]
    loads = [
        pltpu.make_async_copy(w_out, wo_v, w_sem.at[0]),
        pltpu.make_async_copy(w_gate.at[0], wgu.at[:, pl.ds(0, hidden_units)], w_sem.at[1]),
        pltpu.make_async_copy(w_up.at[0], wgu.at[:, pl.ds(hidden_units, hidden_units)], w_sem.at[2]),
    ]
    for k in range(n_tp):
        loads.append(pltpu.make_async_copy(w_down.at[0, :, pl.ds(128 * k, 128)], wd_v.at[k], w_sem.at[3 + k]))
    for load in small:
        load.start()
    disp[...] = jnp.zeros_like(disp)
    ret[...] = jnp.zeros_like(ret)

    barrier = pltpu.get_barrier_semaphore()

    def greet_sp(i, _):
        pl.semaphore_signal(barrier, inc=1, device_id={"sp": lax.rem(b + i, n_sp)}, device_id_type=MESH)
        return 0

    def greet_tp(i, _):
        pl.semaphore_signal(barrier, inc=1, device_id={"tp": lax.rem(p + i, n_tp)}, device_id_type=MESH)
        return 0

    lax.fori_loop(1, n_sp, greet_sp, 0)
    lax.fori_loop(1, n_tp, greet_tp, 0)
    for load in loads:
        load.start()
    for load in small:
        load.wait()

    def to_sp(src, dst, send, recv, who):
        return pltpu.make_async_remote_copy(src, dst, send, recv, device_id={"sp": who}, device_id_type=MESH)

    def to_tp(src, dst, send, recv, who):
        return pltpu.make_async_remote_copy(src, dst, send, recv, device_id={"tp": who}, device_id_type=MESH)

    side = 4
    half, part = slots // 2, slots // 4
    x, y = lax.rem(p, side), lax.div(p, side)
    spots = ((x, y), (y, x))

    def near(v, step):
        return lax.rem(v + side + step, side)

    def place(plan, f, s):
        return s * side + f if plan == 0 else f * side + s

    plans = [(plan, f, s) for plan, (f, s) in enumerate(spots)]

    mark("local")
    low = (iota((tokens, tokens), 0) >= iota((tokens, tokens), 1)).astype(F32)

    def head(q, f, room_ref):
        q = silu(q)
        rate = room_ref[...] / (1.0 + jnp.exp(f))
        cum = dot(low, jnp.log1p(-rate), precision=TOP)
        mid = cum[tokens // 2 - 1 : tokens // 2, :]
        end = cum[tokens - 1 : tokens, :]
        return q * jnp.exp(cum - mid), rate * jnp.exp(mid - cum), q * jnp.exp(cum), rate * jnp.exp(end - cum), end

    near_qw, near_rw, far_qw, far_rw, end_w = head(qw[...].astype(F32), fw[...].astype(F32), room_w)
    near_qn, near_rn, far_qn, far_rn, end_n = head(qn[...].astype(F32).T, fn[...].astype(F32).T, room_n)
    v = val[...].astype(F32)
    v_t = v.T
    s_w = dot(v_t[:DV], far_rw, precision=TOP)
    s_n = dot(v_t[DV:], far_rn, precision=TOP)
    s_n = jnp.concatenate([s_n[: DV // 2], s_n[DV // 2 :]], axis=1)
    states = jnp.concatenate([s_w, s_n], axis=0)
    for j in range(NODE):
        st[j] = states[j * PART : (j + 1) * PART].astype(BF16)
    lg[q] = jnp.concatenate([end_w, jnp.concatenate([end_n, end_n], axis=1)], axis=0)

    mark("barrier")
    pl.semaphore_wait(barrier, n_sp + n_tp - 2)

    mark("d2d")
    def mate(i):
        return lax.rem(q + i, NODE)

    def st_copy(i, who, slot):
        return to_sp(st.at[who], st_in.at[slot], st_send.at[i], st_recv.at[slot], NODE * node + who)

    def lg_copy(i, who, slot):
        return to_sp(lg.at[slot], lg.at[slot], lg_send.at[i], lg_recv.at[slot], NODE * node + who)

    def x_copy(i, who, slot):
        return to_sp(x_src.at[who], x_in.at[slot], x_send.at[i], x_recv.at[slot], NODE * node + who)

    for i in range(1, NODE):
        lg_copy(i, mate(i), q).start()
        st_copy(i, mate(i), q).start()
    st_in[q] = st[q]

    gains[p] = jnp.broadcast_to(gain_n[...], gains.shape[1:])

    def send_gain(i, _):
        who = lax.rem(p + i, n_tp)
        to_tp(gains.at[p], gains.at[p], gain_send.at[i], gain_recv.at[p], who).start()
        return 0

    lax.fori_loop(1, n_tp, send_gain, 0)

    own_rows = iota((PART, 128), 0) + PART * q < DV

    def decay(logs):
        return jnp.exp(jnp.where(own_rows, logs[0:1], logs[1:2]))

    mark("d2dwait")
    for i in range(1, NODE):
        lg_copy(i, mate(i), mate(i)).wait_recv()
        st_copy(i, mate(i), mate(i)).wait_recv()
    decays = [decay(lg[j]) for j in range(NODE)]
    ends = [st_in[j].astype(F32) for j in range(NODE)]
    whole = ends[0]
    for j in range(1, NODE):
        whole = decays[j] * whole + ends[j]
    t_src[...] = whole.astype(BF16)
    l_src[...] = (lg[0] + lg[1]) + (lg[2] + lg[3])

    def t_copy(i, slot):
        return to_sp(t_src, t_buf.at[slot], t_send.at[i], t_recv.at[slot], NODE * i + q)

    def l_copy(i, slot):
        return to_sp(l_src, l_buf.at[slot], l_send.at[i], l_recv.at[slot], NODE * i + q)

    def send_state(i, _):
        l_copy(i, node).start()
        t_copy(i, node).start()
        return 0

    lax.fori_loop(node + 1, nodes, send_state, 0)

    mark("inner")
    def inside(near_q, near_r, content):
        scores = dot(near_q, near_r, ((1,), (1,)), precision=TOP) * low
        return dot(scores, content, precision=TOP)

    out_w = inside(near_qw, near_rw, v[:, :DV])
    out_n = inside(near_qn, near_rn, v[:, DV:])
    gated = gain_h[...] * silu(gate_in[...].astype(F32))

    sub = iota((n_sp, tokens), 0)
    hit0 = (sub == ids[0:1, :]).astype(F32)
    hit1 = (sub == ids[1:2, :]).astype(F32)
    strict = (iota((tokens, tokens), 0) < iota((tokens, tokens), 1)).astype(BF16)
    taken = dot((hit0 + hit1).astype(BF16), strict)
    row0 = ids[0:1, :].astype(F32) * PADCAP + jnp.sum(taken * hit0, axis=0, keepdims=True)
    row1 = ids[1:2, :].astype(F32) * PADCAP + jnp.sum((taken + hit0) * hit1, axis=0, keepdims=True)

    def upright(row):
        return jnp.broadcast_to(row, (tokens, tokens)).T[:, 0:1]

    pos0, pos1, weight0, weight1 = upright(row0), upright(row1), upright(rw[0:1, :]), upright(rw[1:2, :])
    slot = iota((padded, tokens), 0).astype(F32)
    pick = ((slot == row0) | (slot == row1)).astype(BF16)
    column = iota((tokens, padded), 1).astype(F32)
    weigh = jnp.where(column == pos0, weight0, 0.0) + jnp.where(column == pos1, weight1, 0.0)
    weigh_hi = weigh.astype(BF16)
    weigh_lo = (weigh - weigh_hi.astype(F32)).astype(BF16)
    filled = iota((slots, padded), 0).astype(F32)
    filled = filled + (PADCAP - CAP) * jnp.floor((filled + 0.5) * (1.0 / CAP))
    squeeze = (filled == iota((slots, padded), 1).astype(F32)).astype(BF16)
    spread = iota((padded, slots), 1).astype(F32)
    spread = spread + (PADCAP - CAP) * jnp.floor((spread + 0.5) * (1.0 / CAP))
    spread = (spread == iota((padded, slots), 0).astype(F32)).astype(BF16)

    mark("fold")
    def fold(i, carry):
        l_copy(i, i).wait_recv()
        t_copy(i, i).wait_recv()
        return decay(l_buf[i]) * carry + t_buf[i].astype(F32)

    carry = lax.fori_loop(0, node, fold, jnp.zeros((PART, 128), F32))
    for j in range(NODE):
        x_src[j] = carry.astype(BF16)
        if j + 1 < NODE:
            carry = decays[j] * carry + ends[j]
    for i in range(1, NODE):
        x_copy(i, mate(i), q).start()
    x_in[q] = x_src[q]
    mark("xwait")
    for i in range(1, NODE):
        x_copy(i, mate(i), mate(i)).wait_recv()
    mark("mix")
    before = jnp.concatenate([x_in[j].astype(F32) for j in range(NODE)], axis=0)
    in_w = before[:DV]
    in_n = before[DV:]
    in_n = jnp.concatenate([in_n[:, :DKN], in_n[:, DKN:]], axis=0)
    out_w = out_w + dot(far_qw, in_w, ((1,), (1,)), precision=TOP)
    out_n = out_n + dot(far_qn, in_n, ((1,), (1,)), precision=TOP)

    def normed(o):
        return o * lax.rsqrt(jnp.mean(o * o, axis=1, keepdims=True) + EPS)

    mix[p] = (jnp.concatenate([normed(out_w), normed(out_n)], axis=1) * gated).astype(BF16)

    mix_sent = []

    def mix_copy(plan, k, src, who):
        at = mix.at[src, pl.ds(plan * (tokens // 2), tokens // 2)]
        return to_tp(at, at, mix_send.at[plan, k], mix_recv.at[plan, src], who)

    def mix_push(plan, src, who):
        copy = mix_copy(plan, sum(1 for k, _ in mix_sent if k == plan), src, who)
        copy.start()
        mix_sent.append((plan, copy))

    def mix_arrive(plan, src):
        mix_copy(plan, 0, src, lax.rem(p + 1, n_tp)).wait_recv()

    for plan, f, s in plans:
        for step in (2, 1, -1):
            mix_push(plan, p, place(plan, near(f, step), s))
    for plan, f, s in plans:
        for step in (2, 1, -1):
            mix_push(plan, p, place(plan, f, near(s, step)))
    mark("project")
    for step in (1, -1, 2):
        for plan, f, s in plans:
            src = place(plan, near(f, step), s)
            mix_arrive(plan, src)
            for other in (2, 1, -1):
                mix_push(plan, src, place(plan, f, near(s, other)))
    mark("project2")
    loads[0].wait()

    def w_out_rows(src):
        return wo_v[pl.ds(pl.multiple_of(src * 128, 128), 128), :]

    for step in (1, -1, 2):
        for plan, f, s in plans:
            mix_arrive(plan, place(plan, f, near(s, step)))

    def project(sources):
        left = jnp.concatenate([mix[src] for src in sources], axis=1)
        return dot(left, jnp.concatenate([w_out_rows(src) for src in sources], axis=0))

    projected = project([p] + [y * side + near(x, k) for k in (1, 2, 3)] + [near(y, k) * side + x for k in (1, 2, 3)])
    mark("project3")
    for first in (1, -1, 2):
        for step in (1, -1, 2):
            for plan, f, s in plans:
                mix_arrive(plan, place(plan, near(f, first), near(s, step)))
    projected = projected + project([near(y, k) * side + near(x, j) for k in (1, 2, 3) for j in (1, 2, 3)])
    mark("pack")
    mid = (res[...].astype(F32) + projected).astype(BF16)

    packed = dot(pick, mid).astype(BF16)
    disp_src[...] = packed.reshape(n_sp, PADCAP, 128)
    disp[b] = disp_src[b]

    used = pl.ds(0, CAP)

    def disp_copy(i, src, dst, who):
        return to_sp(disp_src.at[src, used], disp.at[dst, used], disp_send.at[i], disp_recv.at[dst], who)

    def ret_copy(i, src, dst, who):
        return to_sp(ret_src.at[src, used], ret.at[dst, used], ret_send.at[i], ret_recv.at[dst], who)

    outward = [lax.rem(b + n_sp // 2, n_sp)]
    for step in range(1, n_sp // 2):
        outward += [lax.rem(b + n_sp // 2 + step, n_sp), lax.rem(b + n_sp // 2 - step, n_sp)]
    for i, who in enumerate(outward):
        disp_copy(i, who, b, who).start()
    mark("dispwait")
    for i, who in enumerate(reversed(outward)):
        disp_copy(i, who, who, who).wait_recv()
    mark("squeeze")
    rows[p] = dot(squeeze, disp[...].reshape(padded, 128)).astype(BF16)

    sent = []

    def row_copy(plan, k, src, q, who):
        at = rows.at[src, pl.ds(plan * half + q * part, part)]
        return to_tp(at, at, rows_send.at[plan, k], rows_recv.at[plan, src, q], who)

    def push(plan, src, q, who):
        copy = row_copy(plan, sum(1 for k, _ in sent if k == plan), src, q, who)
        copy.start()
        sent.append((plan, copy))

    def arrive(plan, src, q):
        row_copy(plan, 0, src, q, lax.rem(p + 1, n_tp)).wait_recv()

    def push_both(plan, src, ahead, behind):
        push(plan, src, 0, ahead)
        push(plan, src, 1, behind)
        push(plan, src, 1, ahead)
        push(plan, src, 0, behind)

    def gate_up(plan, src):
        at = pl.ds(plan * half, half)
        x_in_half = rows[src, at].astype(F32)
        content = (x_in_half * gains[src][0:1]).astype(BF16)
        acc[at, :] += dot(content, wgu[pl.ds(pl.multiple_of(src * 128, 128), 128), :])
        squares[at, :] += x_in_half * x_in_half

    for plan, f, s in plans:
        push_both(plan, p, place(plan, near(f, 1), s), place(plan, near(f, -1), s))
    for plan, f, s in plans:
        push_both(plan, p, place(plan, f, near(s, 1)), place(plan, f, near(s, -1)))
    mark("agown")

    def have_gain(i, _):
        s = lax.rem(p + i, n_tp)
        to_tp(gains.at[s], gains.at[s], gain_send.at[i], gain_recv.at[s], s).wait_recv()
        return 0

    lax.fori_loop(1, n_tp, have_gain, 0)
    for load in loads[1:]:
        load.wait()
    acc[...] = jnp.zeros_like(acc)
    squares[...] = jnp.zeros_like(squares)
    for plan, f, s in plans:
        gate_up(plan, p)
    mark("ag1")
    for plan, f, s in plans:
        for q, step in ((0, -1), (1, 1)):
            src = place(plan, near(f, step), s)
            arrive(plan, src, q)
            push(plan, src, q, place(plan, near(f, -step), s))
    for plan, f, s in plans:
        for q, step in ((0, -1), (1, 1)):
            src = place(plan, near(f, step), s)
            arrive(plan, src, 1 - q)
            push_both(plan, src, place(plan, f, near(s, 1)), place(plan, f, near(s, -1)))
    mark("ag2")

    def pass_on(plan, f, f_from, s):
        for q, step in ((0, -1), (1, 1)):
            src = place(plan, f_from, near(s, step))
            arrive(plan, src, q)
            push(plan, src, q, place(plan, f, near(s, -step)))

    def finish(plan, f_from, s):
        for q, step in ((0, -1), (1, 1)):
            arrive(plan, place(plan, f_from, near(s, step)), 1 - q)
            gate_up(plan, place(plan, f_from, near(s, step)))

    for plan, f, s in plans:
        pass_on(plan, f, f, s)
    for plan, f, s in plans:
        for step in (-1, 1):
            gate_up(plan, place(plan, near(f, step), s))
    mark("ag3")
    for q in (0, 1):
        for plan, f, s in plans:
            src = place(plan, near(f, 2), s)
            arrive(plan, src, q)
            step = 1 - 2 * q
            push(plan, src, q, place(plan, f, near(s, step)))
            push(plan, src, q, place(plan, f, near(s, -step)))
    for plan, f, s in plans:
        finish(plan, f, s)
    mark("ag4")
    for plan, f, s in plans:
        pass_on(plan, f, near(f, -1), s)
        pass_on(plan, f, near(f, 1), s)
    for plan, f, s in plans:
        gate_up(plan, place(plan, near(f, 2), s))
        finish(plan, near(f, -1), s)
    mark("ag5")
    for plan, f, s in plans:
        pass_on(plan, f, near(f, 2), s)
    for plan, f, s in plans:
        finish(plan, near(f, 1), s)
        finish(plan, near(f, 2), s)
    mark("ag6")
    for step in (0, -1, 1, 2):
        for plan, f, s in plans:
            src = place(plan, near(f, step), near(s, 2))
            arrive(plan, src, 0)
            arrive(plan, src, 1)
            gate_up(plan, src)
    mark("act")
    scale = lax.rsqrt(jnp.sum(squares[...], axis=1, keepdims=True) * (1.0 / D) + EPS)
    hidden = (silu(acc[:, :hidden_units] * scale) * (acc[:, hidden_units:] * scale)).astype(BF16)
    mark("down")

    order = (2, 1, 3, 0)

    def partial(plan, f, s):
        right = jnp.concatenate([wd_v[place(plan, f, near(s, r))] for r in order], axis=1)
        value = dot(hidden[plan * half : (plan + 1) * half], right)
        return [[value[q * part : (q + 1) * part, 128 * k : 128 * k + 128] for k in range(side)] for q in range(2)]

    def heavy_copy(plan, way, kind, k):
        at = plan, way, kind, k
        _, f, s = plans[plan]
        who = place(plan, near(f, 1 - 2 * way), s)
        return to_tp(heavy_src.at[at], heavy.at[at], heavy_send.at[at], heavy_recv.at[at], who)

    def light_copy(plan, k):
        at = plan, k
        _, f, s = plans[plan]
        who = place(plan, f, near(s, order[k]))
        return to_tp(light_src.at[at], light.at[at], light_send.at[at], light_recv.at[at], who)

    both = [(plan, way) for plan in range(2) for way in range(2)]
    for plan, f, s in plans:
        far = partial(plan, near(f, 2), s)
        for k in range(side):
            for way in range(2):
                heavy_src[plan, way, 0, k] = far[way][k].astype(BF16)
                heavy_copy(plan, way, 0, k).start()
    for plan, f, s in plans:
        for way in range(2):
            beside = partial(plan, near(f, 1 - 2 * way), s)
            for k in range(side):
                heavy_src[plan, way, 1, k] = beside[1 - way][k].astype(BF16)
                heavy_copy(plan, way, 1, k).start()
                keep[plan, way, k] = beside[way][k]
    for plan, f, s in plans:
        own = partial(plan, f, s)
        for q in range(2):
            for k in range(side):
                line[plan, q, k] = own[q][k]
    mark("rs1")
    for k in range(side):
        for plan, way in both:
            heavy_copy(plan, way, 0, k).wait_recv()
            heavy_src[plan, way, 2, k] = (keep[plan, way, k] + heavy[plan, way, 0, k].astype(F32)).astype(BF16)
            heavy_copy(plan, way, 2, k).start()
    mark("rs2")
    for k in range(side):
        for plan, way in both:
            heavy_copy(plan, way, 1, k).wait_recv()
            line[plan, 1 - way, k] += heavy[plan, way, 1, k].astype(F32)
    mark("rs3")
    for k in range(side):
        for plan, way in both:
            heavy_copy(plan, way, 2, k).wait_recv()
            line[plan, way, k] += heavy[plan, way, 2, k].astype(F32)
            if k < 3 and way == 1:
                light_src[plan, k] = line[plan, :, k].astype(BF16)
                light_copy(plan, k).start()
    mark("rs4")
    sums = []
    for plan in range(2):
        value = [line[plan, q, 3] for q in range(2)]
        for k in (1, 2, 0):
            light_copy(plan, k).wait_recv()
            value = [value[q] + light[plan, k, q].astype(F32) for q in range(2)]
        sums += value
    total = jnp.concatenate(sums, axis=0).astype(BF16)

    mark("retsend")
    ret_src[...] = dot(spread, total).astype(BF16).reshape(n_sp, PADCAP, 128)
    ret[b] = ret_src[b]

    for i, who in enumerate(outward):
        ret_copy(i, who, b, who).start()
    mark("retwait")
    for i in range(1, NODE):
        st_copy(i, mate(i), q).wait_send()
        lg_copy(i, mate(i), q).wait_send()
        x_copy(i, mate(i), q).wait_send()

    def state_gone(i, _):
        t_copy(i, node).wait_send()
        l_copy(i, node).wait_send()
        return 0

    lax.fori_loop(node + 1, nodes, state_gone, 0)

    def tp_gone(i, _):
        who = lax.rem(p + i, n_tp)
        to_tp(gains.at[p], gains.at[p], gain_send.at[i], gain_recv.at[p], who).wait_send()
        return 0

    lax.fori_loop(1, n_tp, tp_gone, 0)

    for _, copy in mix_sent + sent:
        copy.wait_send()
    for plan in range(2):
        for k in range(side):
            for way in range(2):
                for kind in range(3):
                    heavy_copy(plan, way, kind, k).wait_send()
            if k < 3:
                light_copy(plan, k).wait_send()
    for i, who in enumerate(outward):
        disp_copy(i, who, b, who).wait_send()
    mark("retwait2")
    for i, who in enumerate(reversed(outward)):
        ret_copy(i, who, who, who).wait_recv()
    mark("final")
    back = ret[...].reshape(padded, 128)
    moe = dot(weigh_hi, back) + dot(weigh_lo, back)
    out[...] = (mid.astype(F32) + moe).astype(BF16)

    mark("sendwait")
    for i, who in enumerate(outward):
        ret_copy(i, who, b, who).wait_send()
    mark()


def body(n_sp, n_tp, *args):
    (res, qw, qn, fw, fn, room_w, room_n, val, gate_in, gain_h, w_out, gain_n, ids, rw, w_gate, w_up, w_down) = args
    tokens = res.shape[0]
    hidden = w_gate.shape[2]
    nodes = n_sp // NODE
    slots = n_sp * CAP
    row = lambda a: a.reshape(1, -1)
    hbm = pl.BlockSpec(memory_space=pl.ANY)
    dma = pltpu.SemaphoreType.DMA
    V = pltpu.VMEM
    half, part = slots // 2, slots // 4
    small = [res, qw, qn.T, fw, fn.T, row(room_w), row(room_n), val, gate_in, row(gain_h), row(gain_n), ids.T, rw.T]
    scratch = [
        *[V(a.shape, a.dtype) for a in small], dma((len(small),)),
        V((D, 128), BF16), V((D, 2 * hidden), BF16), V((n_tp, hidden, 128), BF16), dma((3 + n_tp,)),
        V((NODE, PART, 128), BF16), V((NODE, PART, 128), BF16), dma((NODE,)), dma((NODE,)),
        V((NODE, 2, 128), F32), dma((NODE,)), dma((NODE,)),
        V((PART, 128), BF16), V((nodes, PART, 128), BF16), V((2, 128), F32), V((nodes, 2, 128), F32),
        dma((nodes,)), dma((nodes,)), dma((nodes,)), dma((nodes,)),
        V((NODE, PART, 128), BF16), V((NODE, PART, 128), BF16), dma((NODE,)), dma((NODE,)),
        V((n_tp, tokens, 128), BF16), dma((2, n_tp)), dma((2, n_tp)),
        V((n_tp, 8, 128), F32), dma((n_tp,)), dma((n_tp,)),
        V((n_sp, PADCAP, 128), BF16), V((n_sp, PADCAP, 128), BF16), dma((n_sp,)), dma((n_sp,)),
        V((n_tp, slots, 128), BF16), dma((2, 30)), dma((2, n_tp, 2)),
        V((2, 2, 3, 4, part, 128), BF16), V((2, 2, 3, 4, part, 128), BF16), dma((2, 2, 3, 4)), dma((2, 2, 3, 4)),
        V((2, 3, 2, part, 128), BF16), V((2, 3, 2, part, 128), BF16), dma((2, 3)), dma((2, 3)),
        V((2, 2, 4, part, 128), F32), V((2, 2, 4, part, 128), F32),
        V((n_sp, PADCAP, 128), BF16), V((n_sp, PADCAP, 128), BF16), dma((n_sp,)), dma((n_sp,)),
        V((slots, 2 * hidden), F32), V((slots, 128), F32),
    ]
    return pl.pallas_call(
        functools.partial(kernel, n_sp, n_tp, slots),
        out_shape=jax.ShapeDtypeStruct((tokens, 128), BF16),
        in_specs=[hbm] * 17,
        out_specs=pl.BlockSpec(memory_space=pltpu.VMEM),
        scratch_shapes=scratch,
        compiler_params=pltpu.CompilerParams(
            collective_id=0, has_side_effects=True, vmem_limit_bytes=67043328
        ),
    )(*small[:10], w_out, *small[10:], w_gate, w_up, w_down)


def solution(mesh):
    both = P("sp", "tp")
    placed = (
        both, both, both, both, both, P("tp"), P("tp"), both, both, P("tp"), P(None, "tp"), P("tp"),
        P("sp", None), P("sp", None), P("sp", None, "tp"), P("sp", None, "tp"), P("sp", "tp", None),
    )
    fn = functools.partial(body, mesh.shape["sp"], mesh.shape["tp"])
    return jax.shard_map(fn, mesh=mesh, in_specs=placed, out_specs=both, check_vma=False)
```
